32 devices in a mesh: gr: 2 (over x), sp: 8 (over z, y), tp: 2 (over core).
Axes of the slice: x: 2, y: 2, z: 4, core: 2. Of those that a mesh axis runs over, the one named last changes fastest.
Arguments:
- tokens: bfloat16 [8, 1024, 4096], P('gr', 'sp'), parts along dimension 0, may hold values from -6 to 6
- key_weight: bfloat16 [4096, 2048], P('sp', 'tp'), may hold values from -0.09375 to 0.09375
- value_weight: bfloat16 [4096, 2048], P('sp', 'tp'), may hold values from -0.09375 to 0.09375
- log_decay: float32 [32, 8, 1024], P('tp', 'gr', 'sp'), parts along dimension 1, may hold values from -1 to 0, as said below
- new_query: bfloat16 [8, 2048], P('gr', 'tp'), parts along dimension 0, may hold values from -6 to 6
- new_key: bfloat16 [8, 2048], P('gr', 'tp'), parts along dimension 0, may hold values from -24 to 24
- new_value: bfloat16 [8, 2048], P('gr', 'tp'), parts along dimension 0, may hold values from -6 to 6
- step_decay: float32 [32, 8], P('tp', 'gr'), parts along dimension 1, may hold values from -1.5 to -0.05
- norm_gain: float32 [2048], P('tp'), may hold values from 0.1 to 1.9
Outputs:
- state_cache: float32 [512, 32, 64], P('gr', 'tp'), parts along dimension 0
- first_read: bfloat16 [8, 2048], P('gr', 'tp'), parts along dimension 0
The draws below stay inside these ranges and needn't reach their ends.
There are 2 independent parts, one for each index of `gr`. The reference program is written for one: setup_inputs(seed, part) draws one part's arguments, and reference() takes and returns one part's arrays. A program takes and returns all parts, laid end to end along the dimension named above; an argument that names none is the same for every part. Nothing has to cross between parts.
Inputs may be any that keep to these rules, and one draw needn't show every extreme that they name: `log_decay`: every entry is at most zero.
All inputs are finite; a program needn't handle non-finite values.
Results may differ from the reference program's by a relative error of at most 0.0053.
Values may be sent and summed in bfloat16 or wider, within the bound.
A program may use at most 64 MiB of HBM per device.

```python
import jax
import jax.numpy as jnp
from jax import lax

D = 4096
RETENTION_HEADS = 32
HEAD_DIM = 64
GROUP_PROMPTS = 4
SPAN = 128
PROMPT_LENGTH = 1024


def draw_log_decay(key, part):
    key_vectors = jax.random.split(jax.random.fold_in(key, 7), 7)
    fast_share = 0.5
    is_fast = jax.random.uniform(key_vectors[0], (RETENTION_HEADS,), jnp.float32) < fast_share
    fast_rate = jnp.exp(jax.random.uniform(key_vectors[1], (RETENTION_HEADS,), jnp.float32, jnp.log(1.0 / 60.0), jnp.log(1.0 / 30.0)))
    slow_rate = jax.random.uniform(key_vectors[2], (RETENTION_HEADS,), jnp.float32, 0.1, 0.5) * jnp.log(10.0) / PROMPT_LENGTH
    decay_speed = jnp.where(is_fast, fast_rate, slow_rate)
    blocks = PROMPT_LENGTH // SPAN
    block_multiplier = jnp.exp(jax.random.uniform(key_vectors[3], (GROUP_PROMPTS, blocks), jnp.float32, jnp.log(0.5), jnp.log(2.0)))
    block_multiplier = jnp.broadcast_to(block_multiplier[:, :, None], (GROUP_PROMPTS, blocks, SPAN)).reshape(GROUP_PROMPTS, PROMPT_LENGTH)
    approximate = jax.random.uniform(key_vectors[4], (RETENTION_HEADS, GROUP_PROMPTS, PROMPT_LENGTH), jnp.float32, 0.5, 1.5)
    surge_position = jax.random.uniform(key_vectors[5], (RETENTION_HEADS, GROUP_PROMPTS, PROMPT_LENGTH), jnp.float32) < 2.0 / PROMPT_LENGTH
    surge_length = jnp.log(jax.random.uniform(key_vectors[6], (RETENTION_HEADS, GROUP_PROMPTS, PROMPT_LENGTH), jnp.float32, 0.5, 0.8))
    decay_factor = -decay_speed[:, None, None] * block_multiplier[None, :, :] * approximate + jnp.where(surge_position, surge_length, 0.0)
    return decay_factor.astype(jnp.float32)


def shard_levels(rng, dims, shards, smallest, top_value):
    def one(dim, parts):
        draws = jax.random.uniform(jax.random.fold_in(jax.random.fold_in(rng, 6), dim), (parts,), jnp.float32, smallest / len(shards), top_value / len(shards))
        return jnp.repeat(jnp.exp(draws), dims[dim] // parts).reshape((-1,) + (1,) * (len(dims) - dim - 1))

    level = one(*shards[0])
    for cut in shards[1:]:
        level = level * one(*cut)
    return level


def normal_values(own_key, dims, deviation, limit, shards=(), held_as=jnp.bfloat16):
    drawn = deviation * jax.random.normal(own_key, dims, jnp.float32)
    if shards:
        drawn = drawn * shard_levels(own_key, dims, shards, -0.22, 0.18)
    return jnp.clip(drawn, -limit, limit).astype(held_as)


def setup_inputs(seed: int = 0, part: int = 0) -> dict:
    key_list = jax.random.split(jax.random.key(seed), 10)
    part_splits = jax.random.split(jax.random.fold_in(key_list[9], part), 10)
    return {
        "tokens": normal_values(part_splits[0], (GROUP_PROMPTS, PROMPT_LENGTH, D), 1.0, 6.0, ((1, 8),)),
        "key_weight": normal_values(key_list[1], (D, RETENTION_HEADS * HEAD_DIM), D ** -0.5, 0.09375, ((0, 8), (1, 2))),
        "value_weight": normal_values(key_list[2], (D, RETENTION_HEADS * HEAD_DIM), D ** -0.5, 0.09375, ((0, 8), (1, 2))),
        "log_decay": draw_log_decay(jax.random.fold_in(jax.random.fold_in(key_list[9], part), 71), part),
        "new_query": normal_values(part_splits[4], (GROUP_PROMPTS, RETENTION_HEADS * HEAD_DIM), 1.0, 6.0, ((1, 2),)),
        "new_key": normal_values(part_splits[5], (GROUP_PROMPTS, RETENTION_HEADS * HEAD_DIM), 4.0, 24.0, ((1, 2),)),
        "new_value": normal_values(part_splits[6], (GROUP_PROMPTS, RETENTION_HEADS * HEAD_DIM), 1.0, 6.0, ((1, 2),)),
        "step_decay": jnp.clip(-1.5 + 1.45 * jax.random.uniform(part_splits[7], (RETENTION_HEADS, GROUP_PROMPTS), jnp.float32) ** shard_levels(part_splits[7], (RETENTION_HEADS, GROUP_PROMPTS), ((0, 2),), -0.2, 0.2), -1.5, -0.05),
        "norm_gain": jnp.clip(1.0 + 0.18 * jax.random.normal(key_list[8], (RETENTION_HEADS * HEAD_DIM,), jnp.float32), 0.1, 1.9),
    }


def rotate_half(values, positions):
    half = values.shape[-1] // 2
    inverse = 10000.0 ** (-jnp.arange(half, dtype=jnp.float32) * (2.0 / values.shape[-1]))
    angles = positions[..., None] * inverse
    cosine = jnp.cos(angles)
    sine = jnp.sin(angles)
    first, second = (values[..., :half], values[..., half:])
    return jnp.concatenate([first * cosine - second * sine, second * cosine + first * sine], axis=-1)

def reference(tokens, key_weight, value_weight, log_decay, new_query, new_key, new_value, step_decay, norm_gain):
    seqs, length, width = tokens.shape
    heads = key_weight.shape[1] // HEAD_DIM
    token_rows = tokens.reshape(seqs * length, width)
    key_vectors = jnp.dot(token_rows, key_weight, preferred_element_type=jnp.float32).astype(jnp.bfloat16)
    values = jnp.dot(token_rows, value_weight, preferred_element_type=jnp.float32).astype(jnp.bfloat16)
    key_vectors = lax.optimization_barrier(key_vectors).astype(jnp.float32).reshape(seqs, length, heads, HEAD_DIM)
    values = lax.optimization_barrier(values).astype(jnp.float32).reshape(seqs, length, heads, HEAD_DIM)
    positions = jnp.arange(length, dtype=jnp.float32)
    rkeys = rotate_half(key_vectors, positions[None, :, None]) * HEAD_DIM ** (-0.5)
    totals = lax.optimization_barrier(jnp.sum(log_decay, axis=-1, keepdims=True))
    weight = jnp.exp(totals - jnp.cumsum(log_decay, axis=-1))
    weight_seq = jnp.transpose(weight, (1, 2, 0))

    def one_prompt(items):
        key_seq, value_seq, decay_seq = items
        weighted = key_seq * decay_seq[:, :, None]
        return jnp.einsum('tha,thb->hab', weighted, value_seq, precision=lax.Precision.HIGHEST)
    prompt_state = lax.map(one_prompt, (rkeys, values, weight_seq))
    end_pos = jnp.full((seqs, heads), float(length), jnp.float32)
    query = rotate_half(new_query.astype(jnp.float32).reshape(seqs, heads, HEAD_DIM), end_pos)
    key_new = rotate_half(new_key.astype(jnp.float32).reshape(seqs, heads, HEAD_DIM), end_pos) * HEAD_DIM ** (-0.5)
    value_new = new_value.astype(jnp.float32).reshape(seqs, heads, HEAD_DIM)
    state = jnp.exp(step_decay).T[:, :, None, None] * prompt_state + key_new[:, :, :, None] * value_new[:, :, None, :]
    raw = jnp.einsum('sha,shab->shb', query, state, precision=lax.Precision.HIGHEST)
    center = lax.optimization_barrier(jnp.mean(raw, axis=-1, keepdims=True))
    spread = lax.optimization_barrier(jnp.mean(jnp.square(raw - center), axis=-1, keepdims=True))
    normed = (raw - center) * lax.rsqrt(spread + 1e-06) * norm_gain.reshape(heads, HEAD_DIM)
    first_read = normed.reshape(seqs, heads * HEAD_DIM).astype(jnp.bfloat16)
    state_cache = jnp.transpose(state, (0, 2, 1, 3)).reshape(seqs * HEAD_DIM, heads, HEAD_DIM)
    return (state_cache, first_read)
```

```python
import functools

import jax
import jax.numpy as jnp
from jax import lax
from jax.experimental import pallas as pl
from jax.experimental.pallas import tpu as pltpu
from jax.sharding import PartitionSpec as P

HEAD_DIM = 64
SUB = 2
MESH = pl.DeviceIdType.MESH
F32 = jnp.float32
HIGH = lax.Precision.HIGHEST


def kernel(
    sizes,
    tok, kw, vw, ld, tot, cos_ref, sin_ref,
    out,
    toks, w, keys, vals, lds, tots, part, got, full,
    l_sem, tok_s, tok_r, core_s, core_r, yw_s, yw_r, up_s, dn_s, z_r, x_s, x_r,
    ld_s, ld_r, tot_s, tot_r, rs_s, rs_r, ag_s, ag_r, yg_s, yg_r,
):
    n_sp, seqs, span, heads = sizes
    n_a = n_sp // 2
    g, sp, tp = lax.axis_index("gr"), lax.axis_index("sp"), lax.axis_index("tp")
    a, b = sp // 2, sp % 2
    ob = 1 - b
    core = tp % 2
    mate = tp + 1 - 2 * core
    rows, width = tok.shape
    depth = kw.shape[0]
    cols = kw.shape[1] // 2
    piece = depth // SUB
    half = rows // 2
    hs = heads * seqs
    y_peer = (g, a * 2 + ob, tp)
    x_peer = (1 - g, sp, tp)
    core_peer = (g, sp, mate)

    def mine(col_half):
        return pl.ds(pl.multiple_of(col_half * cols, 128), cols)

    def shard_rows(s, q=None):
        if q is None:
            return pl.ds(pl.multiple_of(s * depth, depth), depth)
        return pl.ds(pl.multiple_of(s * depth + q * piece, piece), piece)

    local = [
        pltpu.make_async_copy(kw.at[:, mine(b)], w.at[0, shard_rows(sp)], l_sem.at[0]),
        pltpu.make_async_copy(vw.at[:, mine(b)], w.at[1, shard_rows(sp)], l_sem.at[1]),
        pltpu.make_async_copy(tok, toks.at[b], l_sem.at[2]),
        pltpu.make_async_copy(ld, lds.at[b], l_sem.at[3]),
        pltpu.make_async_copy(tot, tots.at[sp], l_sem.at[4]),
    ]
    for c in local:
        c.start()

    barrier = pltpu.get_barrier_semaphore()

    @pl.loop(1, n_sp)
    def _(k):
        pl.semaphore_signal(barrier, inc=1, device_id=(g, lax.rem(sp + k, n_sp), tp), device_id_type=MESH)

    pl.semaphore_signal(barrier, inc=1, device_id=x_peer, device_id_type=MESH)
    pl.semaphore_signal(barrier, inc=1, device_id=core_peer, device_id_type=MESH)
    pl.semaphore_wait(barrier, n_sp + 1)

    def remote(src, dst, s, r, dev):
        return pltpu.make_async_remote_copy(
            src_ref=src, dst_ref=dst, send_sem=s, recv_sem=r, device_id=dev, device_id_type=MESH
        )

    def yw(m, q):
        src = (kw, vw)[m].at[pl.ds(q * piece, piece), mine(ob)]
        return remote(src, w.at[m, shard_rows(sp, q)], yw_s.at[m, q], yw_r.at[m, q], y_peer)

    half_rows = pl.ds(pl.multiple_of(core * half, half), half)
    ytok = remote(tok.at[half_rows], toks.at[b, half_rows], tok_s, tok_r, y_peer)
    yld = remote(ld, lds.at[b], ld_s, ld_r, y_peer)

    for m in range(2):
        @pl.when(g == m)
        def _():
            for q in range(SUB):
                yw(m, q).start()
            yld.start()
            ytok.start()
            for q in range(SUB):
                yw(1 - m, q).start()

    local[0].wait()
    local[1].wait()

    def zsend(s, q, up):
        ref = w.at[g, shard_rows(s, q)]
        sem = (up_s if up else dn_s).at[s, q]
        return remote(ref, ref, sem, z_r.at[s, q], (g, sp + (2 if up else -2), tp))

    def xsend(s, q):
        ref = w.at[g, shard_rows(s, q)]
        return remote(ref, ref, x_s.at[s, q], x_r.at[s, q], x_peer)

    def xrecv(s, q):
        ref = w.at[1 - g, shard_rows(s, q)]
        return remote(ref, ref, x_s.at[s, q], x_r.at[s, q], x_peer)

    def launch(s, q):
        @pl.when(a < n_a - 1)
        def _():
            zsend(s, q, True).start()

        @pl.when(a > 0)
        def _():
            zsend(s, q, False).start()

    for q in range(SUB):
        launch(sp, q)
    local[4].wait()

    def tsend(k):
        return remote(tots.at[sp], tots.at[sp], tot_s.at[k], tot_r.at[k], (g, lax.rem(sp + k, n_sp), tp))

    @pl.loop(1, n_sp)
    def _(k):
        tsend(k).start()

    for q in range(SUB):
        for m in range(2):
            @pl.when(g == m)
            def _():
                yw(m, q).wait_recv()
        launch(a * 2 + ob, q)

    @pl.loop(1, n_a)
    def _(d):
        for bb in range(2):
            for q in range(SUB):
                below = (a - d) * 2 + (b if bb == 0 else ob)
                above = (a + d) * 2 + (b if bb == 0 else ob)

                @pl.when(a - d >= 0)
                def _():
                    zsend(below, q, True).wait_recv()

                    @pl.when(a < n_a - 1)
                    def _():
                        zsend(below, q, True).start()

                    xsend(below, q).start()

                @pl.when(a + d < n_a)
                def _():
                    zsend(above, q, False).wait_recv()

                    @pl.when(a > 0)
                    def _():
                        zsend(above, q, False).start()

                    xsend(above, q).start()

    ytok_in = remote(toks.at[ob, half_rows], toks.at[ob, half_rows], tok_s, tok_r, y_peer)
    ctok = remote(toks.at[ob, half_rows], toks.at[ob, half_rows], core_s, core_r, core_peer)
    ytok_in.wait_recv()
    ctok.start()
    yld.wait_recv()

    @pl.loop(1, n_sp)
    def _(k):
        tsend(k).wait_recv()

    for c in local[2:4]:
        c.wait()

    pos_t = lax.broadcasted_iota(jnp.int32, (span, span), 0)
    pos_u = lax.broadcasted_iota(jnp.int32, (span, span), 1)
    later_mask = jnp.where(pos_u > pos_t, 1.0, 0.0).astype(F32)
    suffix = []
    for tb in range(2):
        inside = lax.dot_general(
            later_mask, lds[tb], (((1,), (1,)), ((), ())), precision=HIGH, preferred_element_type=F32
        )
        index = a * 2 + tb

        def add(k, total):
            return total + jnp.where(k > index, tots[k], 0.0)

        after = lax.fori_loop(0, n_sp, add, jnp.zeros(tots.shape[1:], F32))
        suffix.append(inside + after[0:1, :hs])
    row_hs = lax.broadcasted_iota(jnp.int32, (hs, cols), 0)
    lane_head = lax.broadcasted_iota(jnp.int32, (hs, cols), 1) // HEAD_DIM + b * (heads // 2)

    ctok.wait_recv()

    @pl.loop(1, n_a)
    def _(d):
        for bb in range(2):
            for q in range(SUB):
                @pl.when(a - d >= 0)
                def _():
                    xrecv((a - d) * 2 + (b if bb == 0 else ob), q).wait_recv()

                @pl.when(a + d < n_a)
                def _():
                    xrecv((a + d) * 2 + (b if bb == 0 else ob), q).wait_recv()

    for q in range(SUB):
        for m in range(2):
            @pl.when(g == m)
            def _():
                yw(1 - m, q).wait_recv()

    tile = min(256, rows)
    for tb in range(2):
        @pl.loop(0, rows // tile)
        def _(r):
            at = pl.ds(pl.multiple_of(r * tile, tile), tile)
            lhs = toks[tb, at, :]
            keys[tb, at, :] = jnp.dot(lhs, w[0], preferred_element_type=F32).astype(jnp.bfloat16)
            vals[tb, at, :] = jnp.dot(lhs, w[1], preferred_element_type=F32).astype(jnp.bfloat16)

    lane = lax.broadcasted_iota(jnp.int32, (span, 128), 1)
    first = lane % HEAD_DIM < HEAD_DIM // 2
    lane_out = lax.broadcasted_iota(jnp.int32, (HEAD_DIM, 128), 1)
    block = seqs * HEAD_DIM // n_a
    for s in range(seqs):
        select = jnp.where(row_hs == lane_head * seqs + s, 1.0, 0.0).astype(F32)
        weights = [
            jnp.exp(jnp.dot(suffix[tb], select, precision=HIGH, preferred_element_type=F32))
            for tb in range(2)
        ]
        for c0 in range(0, cols, 128):
            total = None
            for tb in range(2):
                at = pl.ds(s * span, span)
                u = keys[tb, at, pl.ds(c0, 128)].astype(F32)
                turned = jnp.where(first, pltpu.roll(u, 128 - 32, 1), pltpu.roll(u, 32, 1))
                spot = pl.ds(tb * span, span)
                rk = u * cos_ref[spot, :] + turned * sin_ref[spot, :]
                weighted = (rk * weights[tb][:, c0:c0 + 128]).astype(jnp.bfloat16)
                term = lax.dot_general(
                    weighted, vals[tb, at, pl.ds(c0, 128)], (((0,), (0,)), ((), ())),
                    preferred_element_type=F32,
                )
                total = term if total is None else total + term
            both = jnp.where(lane_out < HEAD_DIM, total[:HEAD_DIM], total[HEAD_DIM:])
            part[pl.ds(s * HEAD_DIM, HEAD_DIM), pl.ds(c0, 128)] = both.astype(jnp.bfloat16)

    def block_of(k):
        return pl.ds(pl.multiple_of(k * block, block), block)

    def rs(k):
        to = lax.rem(a + k, n_a)
        return remote(part.at[block_of(to)], got.at[k], rs_s.at[k], rs_r.at[k], (g, to * 2 + b, tp))

    @pl.loop(1, n_a)
    def _(k):
        rs(k).start()

    @pl.loop(1, n_a)
    def _(k):
        rs(k).wait_recv()

    def gather(k, total):
        return total + got[k].astype(F32)

    reduced = lax.fori_loop(1, n_a, gather, part[block_of(a), :].astype(F32))
    full[b, block_of(a), :] = reduced.astype(jnp.bfloat16)

    def ag(k):
        here = full.at[b, block_of(a)]
        return remote(here, here, ag_s.at[k], ag_r.at[k], (g, lax.rem(a + k, n_a) * 2 + b, tp))

    def ag_in(k):
        here = full.at[b, block_of(lax.rem(a - k + n_a, n_a))]
        return remote(here, here, ag_s.at[k], ag_r.at[k], y_peer)

    def yg(k, bb):
        here = full.at[bb, block_of(lax.rem(a - k + n_a, n_a))]
        return remote(here, here, yg_s.at[k], yg_r.at[k], y_peer)

    @pl.loop(1, n_a)
    def _(k):
        ag(k).start()

    yg(0, b).start()

    @pl.loop(1, n_a)
    def _(k):
        ag_in(k).wait_recv()
        yg(k, b).start()

    @pl.loop(0, n_a)
    def _(k):
        yg(k, ob).wait_recv()

    out[:, 0:cols] = full[0]
    out[:, cols:2 * cols] = full[1]

    @pl.loop(0, n_a)
    def _(k):
        yg(k, b).wait_send()

    @pl.loop(1, n_a)
    def _(k):
        ag(k).wait_send()
        rs(k).wait_send()

    @pl.loop(1, n_sp)
    def _(k):
        tsend(k).wait_send()

    ytok.wait_send()
    yld.wait_send()
    ctok.wait_send()
    for q in range(SUB):
        for m in range(2):
            yw(m, q).wait_send()
        for s in (sp, a * 2 + ob):
            @pl.when(a < n_a - 1)
            def _():
                zsend(s, q, True).wait_send()

            @pl.when(a > 0)
            def _():
                zsend(s, q, False).wait_send()

    @pl.loop(1, n_a)
    def _(d):
        for bb in range(2):
            for q in range(SUB):
                below = (a - d) * 2 + (b if bb == 0 else ob)
                above = (a + d) * 2 + (b if bb == 0 else ob)

                @pl.when(a - d >= 0)
                def _():
                    @pl.when(a < n_a - 1)
                    def _():
                        zsend(below, q, True).wait_send()

                    xsend(below, q).wait_send()

                @pl.when(a + d < n_a)
                def _():
                    @pl.when(a > 0)
                    def _():
                        zsend(above, q, False).wait_send()

                    xsend(above, q).wait_send()


def prompt_states(token_rows, key_weight, value_weight, decays, totals, cos, sin, seqs, span, heads, n_sp):
    rows, width = token_rows.shape
    depth, whole = key_weight.shape
    cols = whole // 2
    n_a = n_sp // 2
    hs = heads * seqs
    state_rows = seqs * HEAD_DIM
    dma = pltpu.SemaphoreType.DMA
    bf16 = jnp.bfloat16
    hbm = pl.BlockSpec(memory_space=pl.ANY)
    vmem = pl.BlockSpec(memory_space=pltpu.VMEM)
    return pl.pallas_call(
        functools.partial(kernel, (n_sp, seqs, span, heads)),
        out_shape=jax.ShapeDtypeStruct((state_rows, whole), bf16),
        in_specs=[hbm, hbm, hbm, hbm, hbm, vmem, vmem],
        out_specs=vmem,
        scratch_shapes=[
            pltpu.VMEM((2, rows, width), bf16),
            pltpu.VMEM((2, n_sp * depth, cols), bf16),
            pltpu.VMEM((2, rows, cols), bf16),
            pltpu.VMEM((2, rows, cols), bf16),
            pltpu.VMEM((2, hs, span), F32),
            pltpu.VMEM((n_sp, 8, 128), F32),
            pltpu.VMEM((state_rows, cols), bf16),
            pltpu.VMEM((n_a, state_rows // n_a, cols), bf16),
            pltpu.VMEM((2, state_rows, cols), bf16),
            dma((5,)), dma, dma, dma, dma,
            dma((2, SUB)), dma((2, SUB)),
            dma((n_sp, SUB)), dma((n_sp, SUB)), dma((n_sp, SUB)),
            dma((n_sp, SUB)), dma((n_sp, SUB)),
            dma, dma, dma((n_sp,)), dma((n_sp,)),
            dma((n_a,)), dma((n_a,)), dma((n_a,)), dma((n_a,)), dma((n_a,)), dma((n_a,)),
        ],
        compiler_params=pltpu.CompilerParams(
            collective_id=0, has_side_effects=True, vmem_limit_bytes=56 * 1024 * 1024
        ),
    )(token_rows, key_weight, value_weight, decays, totals, cos, sin)


def rotate_half(values, positions):
    half = values.shape[-1] // 2
    inverse = 10000.0 ** (-jnp.arange(half, dtype=jnp.float32) * (2.0 / values.shape[-1]))
    angles = positions[..., None] * inverse
    cosine = jnp.cos(angles)
    sine = jnp.sin(angles)
    first, second = (values[..., :half], values[..., half:])
    return jnp.concatenate(
        [first * cosine - second * sine, second * cosine + first * sine], axis=-1
    )


def shards(
    tokens, key_weight, value_weight, log_decay, new_query, new_key, new_value, step_decay, norm_gain
):
    seqs, span, width = tokens.shape
    heads = key_weight.shape[1] // HEAD_DIM
    n_sp = lax.axis_size("sp")
    token_rows = tokens.reshape(seqs * span, width)
    decays = log_decay.reshape(heads * seqs, span)
    totals = jnp.sum(decays, axis=-1)
    totals = jnp.broadcast_to(jnp.pad(totals, (0, 128 - heads * seqs))[None, :], (8, 128))
    start = (lax.axis_index("sp") // 2) * (2 * span)
    positions = (start + jnp.arange(2 * span, dtype=jnp.int32)).astype(jnp.float32)
    half = HEAD_DIM // 2
    inverse = 10000.0 ** (-jnp.arange(half, dtype=jnp.float32) * (2.0 / HEAD_DIM))
    angles = positions[:, None] * inverse[None, :]
    cosine = jnp.cos(angles) * HEAD_DIM ** (-0.5)
    sine = jnp.sin(angles) * HEAD_DIM ** (-0.5)
    cos = jnp.concatenate([cosine] * 4, axis=-1)
    sin = jnp.concatenate([-sine, sine] * 2, axis=-1)
    summed = prompt_states(
        token_rows, key_weight, value_weight, decays, totals, cos, sin, seqs, span, heads, n_sp
    )
    summed = summed.astype(F32).reshape(seqs * HEAD_DIM, heads, HEAD_DIM)
    end_pos = jnp.full((seqs, heads), float(span * n_sp), jnp.float32)
    query = rotate_half(new_query.astype(jnp.float32).reshape(seqs, heads, HEAD_DIM), end_pos)
    key_new = rotate_half(
        new_key.astype(jnp.float32).reshape(seqs, heads, HEAD_DIM), end_pos
    ) * HEAD_DIM ** (-0.5)
    value_new = new_value.astype(jnp.float32).reshape(seqs, heads, HEAD_DIM)
    decay_all = jnp.repeat(jnp.exp(step_decay).T, HEAD_DIM, axis=0)
    key_all = jnp.transpose(key_new, (0, 2, 1)).reshape(seqs * HEAD_DIM, heads)
    value_all = jnp.repeat(value_new, HEAD_DIM, axis=0)
    state_cache = decay_all[:, :, None] * summed + key_all[:, :, None] * value_all
    state_seq = state_cache.reshape(seqs, HEAD_DIM, heads, HEAD_DIM)
    raw = jnp.einsum("sha,sahb->shb", query, state_seq, precision=lax.Precision.HIGHEST)
    center = jnp.mean(raw, axis=-1, keepdims=True)
    spread = jnp.mean(jnp.square(raw - center), axis=-1, keepdims=True)
    normed = (raw - center) * lax.rsqrt(spread + 1e-06) * norm_gain.reshape(heads, HEAD_DIM)
    first_read = normed.reshape(seqs, heads * HEAD_DIM).astype(jnp.bfloat16)
    return (state_cache, first_read)


def solution(mesh):
    placed = (
        P("gr", "sp", None),
        P("sp", "tp"),
        P("sp", "tp"),
        P("tp", "gr", "sp"),
        P("gr", "tp"),
        P("gr", "tp"),
        P("gr", "tp"),
        P("tp", "gr"),
        P("tp"),
    )
    return jax.shard_map(
        shards,
        mesh=mesh,
        in_specs=placed,
        out_specs=(P("gr", "tp", None), P("gr", "tp")),
        check_vma=False,
    )
```

```python
import functools

import jax
import jax.numpy as jnp
import numpy as np
from jax import lax
from jax.experimental import pallas as pl
from jax.experimental.pallas import tpu as pltpu
from jax.sharding import PartitionSpec as P

HEAD_DIM = 64
SUB = 4
MESH = pl.DeviceIdType.MESH
F32 = jnp.float32
HIGH = lax.Precision.HIGHEST


def kernel(
    sizes,
    tok, kw, vw, ld, cos_tab, sin_tab, nq, nk, nv, sd, gain,
    out, read,
    toks, w, kv, acc, lds, tots, part, got, full, cos_ref, sin_ref, ends, qx, outer, decay,
    l_sem, tok_s, tok_r, core_s, core_r, yw_s, yw_r, up_s, dn_s, z_r, x_s, x_r,
    ld_s, ld_r, tot_s, tot_r, rs_s, rs_r, ag_s, ag_r, yg_s, yg_r,
):
    n_sp, seqs, span, heads = sizes
    n_a = n_sp // 2
    g, sp, tp = lax.axis_index("gr"), lax.axis_index("sp"), lax.axis_index("tp")
    a, b = sp // 2, sp % 2
    ob = 1 - b
    core = tp % 2
    mate = tp + 1 - 2 * core
    rows, width = tok.shape
    depth = kw.shape[0]
    cols = kw.shape[1] // 2
    piece = depth // SUB
    half = rows // 2
    hs = heads * seqs
    y_peer = (g, a * 2 + ob, tp)
    x_peer = (1 - g, sp, tp)
    core_peer = (g, sp, mate)

    def mine(col_half):
        return pl.ds(pl.multiple_of(col_half * cols, 128), cols)

    def shard_rows(s, q=None):
        if q is None:
            return pl.ds(pl.multiple_of(s * depth, depth), depth)
        return pl.ds(pl.multiple_of(s * depth + q * piece, piece), piece)

    local = [
        pltpu.make_async_copy(kw.at[:, mine(b)], w.at[0, shard_rows(sp)], l_sem.at[0]),
        pltpu.make_async_copy(vw.at[:, mine(b)], w.at[1, shard_rows(sp)], l_sem.at[1]),
        pltpu.make_async_copy(tok, toks.at[b], l_sem.at[2]),
        pltpu.make_async_copy(ld, lds.at[b], l_sem.at[3]),
        pltpu.make_async_copy(cos_tab.at[pl.ds(pl.multiple_of(a * 2 * span, 8), 2 * span)], cos_ref, l_sem.at[4]),
        pltpu.make_async_copy(sin_tab.at[pl.ds(pl.multiple_of(a * 2 * span, 8), 2 * span)], sin_ref, l_sem.at[5]),
        pltpu.make_async_copy(cos_tab.at[pl.ds(n_sp * span, 8)], ends.at[0], l_sem.at[6]),
        pltpu.make_async_copy(sin_tab.at[pl.ds(n_sp * span, 8)], ends.at[1], l_sem.at[7]),
    ]
    for c in local:
        c.start()

    barrier = pltpu.get_barrier_semaphore()

    @pl.loop(1, n_sp)
    def _(k):
        pl.semaphore_signal(barrier, inc=1, device_id=(g, lax.rem(sp + k, n_sp), tp), device_id_type=MESH)

    pl.semaphore_signal(barrier, inc=1, device_id=x_peer, device_id_type=MESH)
    pl.semaphore_signal(barrier, inc=1, device_id=core_peer, device_id_type=MESH)
    pl.semaphore_wait(barrier, n_sp + 1)

    def remote(src, dst, s, r, dev):
        return pltpu.make_async_remote_copy(
            src_ref=src, dst_ref=dst, send_sem=s, recv_sem=r, device_id=dev, device_id_type=MESH
        )

    def yw(m, q):
        src = (kw, vw)[m].at[pl.ds(q * piece, piece), mine(ob)]
        return remote(src, w.at[m, shard_rows(sp, q)], yw_s.at[m, q], yw_r.at[m, q], y_peer)

    half_rows = pl.ds(pl.multiple_of(core * half, half), half)
    ytok = remote(tok.at[half_rows], toks.at[b, half_rows], tok_s, tok_r, y_peer)
    yld = remote(ld, lds.at[b], ld_s, ld_r, y_peer)

    for m in range(2):
        @pl.when(g == m)
        def _():
            for q in range(SUB):
                yw(m, q).start()
            yld.start()
            ytok.start()
            for q in range(SUB):
                yw(1 - m, q).start()

    local[0].wait()
    local[1].wait()

    def zsend(s, q, up):
        ref = w.at[g, shard_rows(s, q)]
        sem = (up_s if up else dn_s).at[s, q]
        return remote(ref, ref, sem, z_r.at[s, q], (g, sp + (2 if up else -2), tp))

    def xsend(s, q):
        ref = w.at[g, shard_rows(s, q)]
        return remote(ref, ref, x_s.at[s, q], x_r.at[s, q], x_peer)

    def xrecv(s, q):
        ref = w.at[1 - g, shard_rows(s, q)]
        return remote(ref, ref, x_s.at[s, q], x_r.at[s, q], x_peer)

    def launch(s, q):
        @pl.when(a < n_a - 1)
        def _():
            zsend(s, q, True).start()

        @pl.when(a > 0)
        def _():
            zsend(s, q, False).start()

    for q in range(SUB):
        launch(sp, q)

    def tsend(k):
        return remote(tots.at[sp], tots.at[sp], tot_s.at[k], tot_r.at[k], (g, lax.rem(sp + k, n_sp), tp))

    for c in local[2:]:
        c.wait()
    tots[sp] = jnp.zeros(tots.shape[1:], F32)
    tots[sp, :, 0:hs] = lax.dot_general(
        jnp.ones((8, span), F32), lds[b], (((1,), (1,)), ((), ())), precision=HIGH, preferred_element_type=F32
    )

    lanes = lax.broadcasted_iota(jnp.int32, (HEAD_DIM, 128), 1)
    subs = lax.broadcasted_iota(jnp.int32, (HEAD_DIM, 128), 0)
    diagonal = lanes % HEAD_DIM == subs
    same_head = jnp.where(
        lax.broadcasted_iota(jnp.int32, (128, 128), 0) // HEAD_DIM
        == lax.broadcasted_iota(jnp.int32, (128, 128), 1) // HEAD_DIM, 1.0, 0.0
    ).astype(F32)

    def exact(x, y):
        return jnp.dot(x, y, precision=HIGH, preferred_element_type=F32)

    def at_end(u):
        low = lax.broadcasted_iota(jnp.int32, u.shape, 1) % HEAD_DIM < HEAD_DIM // 2
        turned = jnp.where(low, pltpu.roll(u, 128 - 32, 1), pltpu.roll(u, 32, 1))
        return u * ends[0, 0:1, :] + turned * ends[1, 0:1, :]

    head_lane = lax.broadcasted_iota(jnp.int32, (heads, 2 * cols), 1) // HEAD_DIM
    head_row = lax.broadcasted_iota(jnp.int32, (heads, 2 * cols), 0)
    spread_heads = jnp.where(head_lane == head_row, 1.0, 0.0).astype(F32)
    decay[...] = jnp.exp(exact(sd[...], spread_heads))

    def new_token(c0):
        chunk = pl.ds(c0, 128)
        query = at_end(nq[:, chunk].astype(F32)) * HEAD_DIM ** 0.5
        key_new = at_end(nk[:, chunk].astype(F32))
        value_new = nv[:, chunk].astype(F32)
        for s in range(seqs):
            at = pl.ds(s * HEAD_DIM, HEAD_DIM)
            qx[at, chunk] = exact(jnp.where(diagonal, query[s:s + 1], 0.0), same_head)
            column = exact(jnp.where(diagonal, key_new[s:s + 1], 0.0), same_head)
            outer[at, chunk] = column * value_new[s:s + 1]

    def zstep(d, bb, q):
        below = (a - d) * 2 + (b if bb == 0 else ob)
        above = (a + d) * 2 + (b if bb == 0 else ob)

        @pl.when(a - d >= 0)
        def _():
            zsend(below, q, True).wait_recv()

            @pl.when(a < n_a - 1)
            def _():
                zsend(below, q, True).start()

            xsend(below, q).start()

        @pl.when(a + d < n_a)
        def _():
            zsend(above, q, False).wait_recv()

            @pl.when(a > 0)
            def _():
                zsend(above, q, False).start()

            xsend(above, q).start()

    chunks = list(range(0, 2 * cols, 128))
    for q in range(SUB):
        for m in range(2):
            @pl.when(g == m)
            def _():
                yw(m, q).wait_recv()
        launch(a * 2 + ob, q)
        zstep(1, 0, q)
        for c0 in chunks[q::SUB]:
            new_token(c0)

    @pl.loop(1, n_sp)
    def _(k):
        tsend(k).start()

    tile = min(256, rows)

    def own_product(m, s, fresh=False):
        depth_at = shard_rows(s)

        @pl.loop(0, rows // tile)
        def _(r):
            at = pl.ds(pl.multiple_of(r * tile, tile), tile)
            new = jnp.dot(toks[b, at, depth_at], w[m, depth_at, :], preferred_element_type=F32)
            acc[m, at, :] = new if fresh else acc[m, at, :] + new

    own_product(0, sp, True)
    own_product(1, sp, True)
    own_product(g, a * 2 + ob)

    def take(d, bb, mats):
        side = b if bb == 0 else ob
        for inside, s in ((a - d >= 0, (a - d) * 2 + side), (a + d < n_a, (a + d) * 2 + side)):
            @pl.when(inside)
            def _():
                if 0 in mats:
                    own_product(g, s)
                if 1 in mats:
                    for q in range(SUB):
                        xrecv(s, q).wait_recv()
                    own_product(1 - g, s)

    for q in range(SUB):
        zstep(1, 1, q)

    @pl.loop(2, n_a)
    def _(d):
        for bb in range(2):
            for q in range(SUB):
                zstep(d, bb, q)
            take(d - 1, bb, (0, 1))

    ytok_in = remote(toks.at[ob, half_rows], toks.at[ob, half_rows], tok_s, tok_r, y_peer)
    ctok = remote(toks.at[ob, half_rows], toks.at[ob, half_rows], core_s, core_r, core_peer)
    ytok_in.wait_recv()
    ctok.start()
    yld.wait_recv()

    @pl.loop(1, n_sp)
    def _(k):
        tsend(k).wait_recv()

    pos_t = lax.broadcasted_iota(jnp.int32, (span, span), 0)
    pos_u = lax.broadcasted_iota(jnp.int32, (span, span), 1)
    later_mask = jnp.where(pos_u > pos_t, 1.0, 0.0).astype(F32)
    suffix = []
    for tb in range(2):
        inside = lax.dot_general(
            later_mask, lds[tb], (((1,), (1,)), ((), ())), precision=HIGH, preferred_element_type=F32
        )
        index = a * 2 + tb

        def add(k, total):
            return total + jnp.where(k > index, tots[k], 0.0)

        after = lax.fori_loop(0, n_sp, add, jnp.zeros(tots.shape[1:], F32))
        suffix.append(inside + after[0:1, :hs])
    row_hs = lax.broadcasted_iota(jnp.int32, (hs, cols), 0)
    lane_head = lax.broadcasted_iota(jnp.int32, (hs, cols), 1) // HEAD_DIM + b * (heads // 2)

    def partner_product(m):
        @pl.loop(0, rows // tile)
        def _(r):
            at = pl.ds(pl.multiple_of(r * tile, tile), tile)
            new = jnp.dot(toks[ob, at, :], w[m], preferred_element_type=F32)
            kv[m, ob, at, :] = new.astype(jnp.bfloat16)
            kv[m, b, at, :] = acc[m, at, :].astype(jnp.bfloat16)

    for bb in range(2):
        take(n_a - 1, bb, (0,))
    ctok.wait_recv()
    partner_product(g)
    for q in range(SUB):
        for m in range(2):
            @pl.when(g == m)
            def _():
                yw(1 - m, q).wait_recv()
    own_product(1 - g, a * 2 + ob)
    for bb in range(2):
        take(n_a - 1, bb, (1,))
    partner_product(1 - g)

    lane = lax.broadcasted_iota(jnp.int32, (span, 128), 1)
    first = lane % HEAD_DIM < HEAD_DIM // 2
    lane_out = lax.broadcasted_iota(jnp.int32, (HEAD_DIM, 128), 1)
    block = seqs * HEAD_DIM // n_a
    for s in range(seqs):
        select = jnp.where(row_hs == lane_head * seqs + s, 1.0, 0.0).astype(F32)
        weights = [
            jnp.exp(jnp.dot(suffix[tb], select, precision=HIGH, preferred_element_type=F32))
            for tb in range(2)
        ]
        for c0 in range(0, cols, 128):
            total = None
            for tb in range(2):
                at = pl.ds(s * span, span)
                u = kv[0, tb, at, pl.ds(c0, 128)].astype(F32)
                turned = jnp.where(first, pltpu.roll(u, 128 - 32, 1), pltpu.roll(u, 32, 1))
                spot = pl.ds(tb * span, span)
                rk = u * cos_ref[spot, :] + turned * sin_ref[spot, :]
                weighted = (rk * weights[tb][:, c0:c0 + 128]).astype(jnp.bfloat16)
                term = lax.dot_general(
                    weighted, kv[1, tb, at, pl.ds(c0, 128)], (((0,), (0,)), ((), ())),
                    preferred_element_type=F32,
                )
                total = term if total is None else total + term
            both = jnp.where(lane_out < HEAD_DIM, total[:HEAD_DIM], total[HEAD_DIM:])
            part[pl.ds(s * HEAD_DIM, HEAD_DIM), pl.ds(c0, 128)] = both.astype(jnp.bfloat16)

    def block_of(k):
        return pl.ds(pl.multiple_of(k * block, block), block)

    def rs(k):
        to = lax.rem(a + k, n_a)
        return remote(part.at[block_of(to)], got.at[k], rs_s.at[k], rs_r.at[k], (g, to * 2 + b, tp))

    @pl.loop(1, n_a)
    def _(k):
        rs(k).start()

    @pl.loop(1, n_a)
    def _(k):
        rs(k).wait_recv()

    def gather(k, total):
        return total + got[k].astype(F32)

    reduced = lax.fori_loop(1, n_a, gather, part[block_of(a), :].astype(F32))
    full[b, block_of(a), :] = reduced.astype(jnp.bfloat16)

    def ag(k):
        here = full.at[b, block_of(a)]
        return remote(here, here, ag_s.at[k], ag_r.at[k], (g, lax.rem(a + k, n_a) * 2 + b, tp))

    def ag_in(k):
        here = full.at[b, block_of(lax.rem(a - k + n_a, n_a))]
        return remote(here, here, ag_s.at[k], ag_r.at[k], y_peer)

    def yg(k, bb):
        here = full.at[bb, block_of(lax.rem(a - k + n_a, n_a))]
        return remote(here, here, yg_s.at[k], yg_r.at[k], y_peer)

    @pl.loop(1, n_a)
    def _(k):
        ag(k).start()

    yg(0, b).start()

    @pl.loop(1, n_a)
    def _(k):
        ag_in(k).wait_recv()
        yg(k, b).start()

    @pl.loop(0, n_a)
    def _(k):
        yg(k, ob).wait_recv()

    for c0 in range(0, 2 * cols, 128):
        chunk = pl.ds(c0, 128)
        raws, states = [], []
        for s in range(seqs):
            at = pl.ds(s * HEAD_DIM, HEAD_DIM)
            summed = full[c0 // cols, at, pl.ds(c0 % cols, 128)].astype(F32)
            state = decay[s:s + 1, chunk] * summed + outer[at, chunk]
            raws.append(jnp.sum(qx[at, chunk] * state, axis=0, keepdims=True))
            states.append(state)
        out[chunk, :] = jnp.concatenate(states, axis=0).T
        raw = jnp.concatenate(raws, axis=0)
        center = exact(raw, same_head) * (1.0 / HEAD_DIM)
        off = raw - center
        spread = exact(off * off, same_head) * (1.0 / HEAD_DIM)
        read[:, chunk] = (off * lax.rsqrt(spread + 1e-06) * gain[:, chunk]).astype(jnp.bfloat16)

    @pl.loop(0, n_a)
    def _(k):
        yg(k, b).wait_send()

    @pl.loop(1, n_a)
    def _(k):
        ag(k).wait_send()
        rs(k).wait_send()

    @pl.loop(1, n_sp)
    def _(k):
        tsend(k).wait_send()

    ytok.wait_send()
    yld.wait_send()
    ctok.wait_send()
    for q in range(SUB):
        for m in range(2):
            yw(m, q).wait_send()
        for s in (sp, a * 2 + ob):
            @pl.when(a < n_a - 1)
            def _():
                zsend(s, q, True).wait_send()

            @pl.when(a > 0)
            def _():
                zsend(s, q, False).wait_send()

    @pl.loop(1, n_a)
    def _(d):
        for bb in range(2):
            for q in range(SUB):
                below = (a - d) * 2 + (b if bb == 0 else ob)
                above = (a + d) * 2 + (b if bb == 0 else ob)

                @pl.when(a - d >= 0)
                def _():
                    @pl.when(a < n_a - 1)
                    def _():
                        zsend(below, q, True).wait_send()

                    xsend(below, q).wait_send()

                @pl.when(a + d < n_a)
                def _():
                    @pl.when(a > 0)
                    def _():
                        zsend(above, q, False).wait_send()

                    xsend(above, q).wait_send()


def prompt_states(token_rows, key_weight, value_weight, decays, cos, sin, step, seqs, span, heads, n_sp):
    rows, width = token_rows.shape
    depth, whole = key_weight.shape
    cols = whole // 2
    n_a = n_sp // 2
    hs = heads * seqs
    state_rows = seqs * HEAD_DIM
    dma = pltpu.SemaphoreType.DMA
    bf16 = jnp.bfloat16
    hbm = pl.BlockSpec(memory_space=pl.ANY)
    vmem = pl.BlockSpec(memory_space=pltpu.VMEM)
    return pl.pallas_call(
        functools.partial(kernel, (n_sp, seqs, span, heads)),
        out_shape=(
            jax.ShapeDtypeStruct((whole, state_rows), F32),
            jax.ShapeDtypeStruct((seqs, whole), bf16),
        ),
        in_specs=[hbm] * 6 + [vmem] * 5,
        out_specs=(vmem, vmem),
        scratch_shapes=[
            pltpu.VMEM((2, rows, width), bf16),
            pltpu.VMEM((2, n_sp * depth, cols), bf16),
            pltpu.VMEM((2, 2, rows, cols), bf16),
            pltpu.VMEM((2, rows, cols), F32),
            pltpu.VMEM((2, hs, span), F32),
            pltpu.VMEM((n_sp, 8, 128), F32),
            pltpu.VMEM((state_rows, cols), bf16),
            pltpu.VMEM((n_a, state_rows // n_a, cols), bf16),
            pltpu.VMEM((2, state_rows, cols), bf16),
            pltpu.VMEM((2 * span, 128), F32),
            pltpu.VMEM((2 * span, 128), F32),
            pltpu.VMEM((2, 8, 128), F32),
            pltpu.VMEM((state_rows, whole), F32),
            pltpu.VMEM((state_rows, whole), F32),
            pltpu.VMEM((seqs, whole), F32),
            dma((8,)), dma, dma, dma, dma,
            dma((2, SUB)), dma((2, SUB)),
            dma((n_sp, SUB)), dma((n_sp, SUB)), dma((n_sp, SUB)),
            dma((n_sp, SUB)), dma((n_sp, SUB)),
            dma, dma, dma((n_sp,)), dma((n_sp,)),
            dma((n_a,)), dma((n_a,)), dma((n_a,)), dma((n_a,)), dma((n_a,)), dma((n_a,)),
        ],
        compiler_params=pltpu.CompilerParams(
            collective_id=0, has_side_effects=True, vmem_limit_bytes=56 * 1024 * 1024
        ),
    )(token_rows, key_weight, value_weight, decays, cos, sin, *step)


def position_tables(length):
    half = HEAD_DIM // 2
    inverse = np.float32(10000.0) ** (-np.arange(half, dtype=np.float32) * np.float32(2.0 / HEAD_DIM))
    angles = np.arange(length + 8, dtype=np.float32)[:, None] * inverse[None, :].astype(np.float32)
    cosine = np.cos(angles.astype(np.float64)) * HEAD_DIM ** -0.5
    sine = np.sin(angles.astype(np.float64)) * HEAD_DIM ** -0.5
    cos = np.concatenate([cosine] * 4, axis=-1).astype(np.float32)
    sin = np.concatenate([-sine, sine] * 2, axis=-1).astype(np.float32)
    return cos, sin


def shards(
    tokens, key_weight, value_weight, log_decay, new_query, new_key, new_value, step_decay, norm_gain
):
    seqs, span, width = tokens.shape
    heads = key_weight.shape[1] // HEAD_DIM
    n_sp = lax.axis_size("sp")
    token_rows = tokens.reshape(seqs * span, width)
    decays = log_decay.reshape(heads * seqs, span)
    cos, sin = position_tables(span * n_sp)
    step = (new_query, new_key, new_value, step_decay.T, norm_gain.reshape(1, -1))
    state, read = prompt_states(
        token_rows, key_weight, value_weight, decays, jnp.asarray(cos), jnp.asarray(sin), step,
        seqs, span, heads, n_sp,
    )
    return (state.T.reshape(seqs * HEAD_DIM, heads, HEAD_DIM), read)


def solution(mesh):
    placed = (
        P("gr", "sp", None),
        P("sp", "tp"),
        P("sp", "tp"),
        P("tp", "gr", "sp"),
        P("gr", "tp"),
        P("gr", "tp"),
        P("gr", "tp"),
        P("tp", "gr"),
        P("tp"),
    )
    return jax.shard_map(
        shards,
        mesh=mesh,
        in_specs=placed,
        out_specs=(P("gr", "tp", None), P("gr", "tp")),
        check_vma=False,
    )
```

```python
import functools

import jax
import jax.numpy as jnp
import numpy as np
from jax import lax
from jax.experimental import pallas as pl
from jax.experimental.pallas import tpu as pltpu
from jax.sharding import PartitionSpec as P

HEAD_DIM = 64
SUB = 4
MESH = pl.DeviceIdType.MESH
F32 = jnp.float32
HIGH = lax.Precision.HIGHEST


def kernel(
    sizes,
    tok, kw, vw, ld, cos_tab, sin_tab, nq, nk, nv, sd, gain,
    out, read,
    toks, w, kv, acc, lds, tots, part, got, full, cos_ref, sin_ref, ends, qx, outer, decay, wts,
    l_sem, tok_s, tok_r, core_s, core_r, yw_s, yw_r, up_s, dn_s, z_r, x_s, x_r,
    ld_s, ld_r, tot_s, tot_r, rs_s, rs_r, ag_s, ag_r, yg_s, yg_r,
):
    n_sp, seqs, span, heads = sizes
    n_a = n_sp // 2
    g, sp, tp = lax.axis_index("gr"), lax.axis_index("sp"), lax.axis_index("tp")
    a, b = sp // 2, sp % 2
    ob = 1 - b
    core = tp % 2
    mate = tp + 1 - 2 * core
    rows, width = tok.shape
    depth = kw.shape[0]
    cols = kw.shape[1] // 2
    piece = depth // SUB
    half = rows // 2
    hs = heads * seqs
    y_peer = (g, a * 2 + ob, tp)
    x_peer = (1 - g, sp, tp)
    core_peer = (g, sp, mate)

    def mine(col_half):
        return pl.ds(pl.multiple_of(col_half * cols, 128), cols)

    def shard_rows(s, q=None):
        if q is None:
            return pl.ds(pl.multiple_of(s * depth, depth), depth)
        return pl.ds(pl.multiple_of(s * depth + q * piece, piece), piece)

    local = [
        pltpu.make_async_copy(kw.at[:, mine(b)], w.at[0, shard_rows(sp)], l_sem.at[0]),
        pltpu.make_async_copy(vw.at[:, mine(b)], w.at[1, shard_rows(sp)], l_sem.at[1]),
        pltpu.make_async_copy(tok, toks.at[b], l_sem.at[2]),
        pltpu.make_async_copy(ld, lds.at[b], l_sem.at[3]),
        pltpu.make_async_copy(cos_tab.at[pl.ds(pl.multiple_of(a * 2 * span, 8), 2 * span)], cos_ref, l_sem.at[4]),
        pltpu.make_async_copy(sin_tab.at[pl.ds(pl.multiple_of(a * 2 * span, 8), 2 * span)], sin_ref, l_sem.at[5]),
        pltpu.make_async_copy(cos_tab.at[pl.ds(n_sp * span, 8)], ends.at[0], l_sem.at[6]),
        pltpu.make_async_copy(sin_tab.at[pl.ds(n_sp * span, 8)], ends.at[1], l_sem.at[7]),
    ]
    for c in local:
        c.start()

    barrier = pltpu.get_barrier_semaphore()

    @pl.loop(1, n_sp)
    def _(k):
        pl.semaphore_signal(barrier, inc=1, device_id=(g, lax.rem(sp + k, n_sp), tp), device_id_type=MESH)

    pl.semaphore_signal(barrier, inc=1, device_id=x_peer, device_id_type=MESH)
    pl.semaphore_signal(barrier, inc=1, device_id=core_peer, device_id_type=MESH)
    pl.semaphore_wait(barrier, n_sp + 1)

    def remote(src, dst, s, r, dev):
        return pltpu.make_async_remote_copy(
            src_ref=src, dst_ref=dst, send_sem=s, recv_sem=r, device_id=dev, device_id_type=MESH
        )

    def yw(m, q):
        src = (kw, vw)[m].at[pl.ds(q * piece, piece), mine(ob)]
        return remote(src, w.at[m, shard_rows(sp, q)], yw_s.at[m, q], yw_r.at[m, q], y_peer)

    half_rows = pl.ds(pl.multiple_of(core * half, half), half)
    ytok = remote(tok.at[half_rows], toks.at[b, half_rows], tok_s, tok_r, y_peer)
    yld = remote(ld, lds.at[b], ld_s, ld_r, y_peer)

    for m in range(2):
        @pl.when(g == m)
        def _():
            for q in range(SUB):
                yw(m, q).start()
            yld.start()
            ytok.start()
            for q in range(SUB):
                yw(1 - m, q).start()

    local[0].wait()
    local[1].wait()

    def zsend(s, q, up):
        ref = w.at[g, shard_rows(s, q)]
        sem = (up_s if up else dn_s).at[s, q]
        return remote(ref, ref, sem, z_r.at[s, q], (g, sp + (2 if up else -2), tp))

    def xsend(s, q):
        ref = w.at[g, shard_rows(s, q)]
        return remote(ref, ref, x_s.at[s, q], x_r.at[s, q], x_peer)

    def xrecv(s, q):
        ref = w.at[1 - g, shard_rows(s, q)]
        return remote(ref, ref, x_s.at[s, q], x_r.at[s, q], x_peer)

    def launch(s, q):
        @pl.when(a < n_a - 1)
        def _():
            zsend(s, q, True).start()

        @pl.when(a > 0)
        def _():
            zsend(s, q, False).start()

    for q in range(SUB):
        launch(sp, q)

    def tsend(k):
        return remote(tots.at[sp], tots.at[sp], tot_s.at[k], tot_r.at[k], (g, lax.rem(sp + k, n_sp), tp))

    for c in local[2:]:
        c.wait()
    tots[sp] = jnp.zeros(tots.shape[1:], F32)
    tots[sp, :, 0:hs] = lax.dot_general(
        jnp.ones((8, span), F32), lds[b], (((1,), (1,)), ((), ())), precision=HIGH, preferred_element_type=F32
    )

    lanes = lax.broadcasted_iota(jnp.int32, (HEAD_DIM, 128), 1)
    subs = lax.broadcasted_iota(jnp.int32, (HEAD_DIM, 128), 0)
    diagonal = lanes % HEAD_DIM == subs
    same_head = jnp.where(
        lax.broadcasted_iota(jnp.int32, (128, 128), 0) // HEAD_DIM
        == lax.broadcasted_iota(jnp.int32, (128, 128), 1) // HEAD_DIM, 1.0, 0.0
    ).astype(F32)

    def exact(x, y):
        return jnp.dot(x, y, precision=HIGH, preferred_element_type=F32)

    def at_end(u):
        low = lax.broadcasted_iota(jnp.int32, u.shape, 1) % HEAD_DIM < HEAD_DIM // 2
        turned = jnp.where(low, pltpu.roll(u, 128 - 32, 1), pltpu.roll(u, 32, 1))
        return u * ends[0, 0:1, :] + turned * ends[1, 0:1, :]

    head_lane = lax.broadcasted_iota(jnp.int32, (heads, 2 * cols), 1) // HEAD_DIM
    head_row = lax.broadcasted_iota(jnp.int32, (heads, 2 * cols), 0)
    spread_heads = jnp.where(head_lane == head_row, 1.0, 0.0).astype(F32)
    decay[...] = jnp.exp(exact(sd[...], spread_heads))

    def new_token(c0):
        chunk = pl.ds(c0, 128)
        query = at_end(nq[:, chunk].astype(F32)) * HEAD_DIM ** 0.5
        key_new = at_end(nk[:, chunk].astype(F32))
        value_new = nv[:, chunk].astype(F32)
        for s in range(seqs):
            at = pl.ds(s * HEAD_DIM, HEAD_DIM)
            qx[at, chunk] = exact(jnp.where(diagonal, query[s:s + 1], 0.0), same_head)
            column = exact(jnp.where(diagonal, key_new[s:s + 1], 0.0), same_head)
            outer[at, chunk] = column * value_new[s:s + 1]

    def zstep(d, bb, q):
        below = (a - d) * 2 + (b if bb == 0 else ob)
        above = (a + d) * 2 + (b if bb == 0 else ob)

        @pl.when(a - d >= 0)
        def _():
            zsend(below, q, True).wait_recv()

            @pl.when(a < n_a - 1)
            def _():
                zsend(below, q, True).start()

            xsend(below, q).start()

        @pl.when(a + d < n_a)
        def _():
            zsend(above, q, False).wait_recv()

            @pl.when(a > 0)
            def _():
                zsend(above, q, False).start()

            xsend(above, q).start()

    chunks = list(range(0, 2 * cols, 128))
    for q in range(SUB):
        for m in range(2):
            @pl.when(g == m)
            def _():
                yw(m, q).wait_recv()
        launch(a * 2 + ob, q)
        zstep(1, 0, q)
        for c0 in chunks[q::SUB]:
            new_token(c0)

    @pl.loop(1, n_sp)
    def _(k):
        tsend(k).start()

    tile = min(256, rows)

    def own_product(m, s, fresh=False):
        depth_at = shard_rows(s)

        @pl.loop(0, rows // tile)
        def _(r):
            at = pl.ds(pl.multiple_of(r * tile, tile), tile)
            new = jnp.dot(toks[b, at, depth_at], w[m, depth_at, :], preferred_element_type=F32)
            acc[m, at, :] = new if fresh else acc[m, at, :] + new

    own_product(0, sp, True)
    own_product(1, sp, True)
    own_product(g, a * 2 + ob)

    def take(d, bb, mats):
        side = b if bb == 0 else ob
        for inside, s in ((a - d >= 0, (a - d) * 2 + side), (a + d < n_a, (a + d) * 2 + side)):
            @pl.when(inside)
            def _():
                if 0 in mats:
                    own_product(g, s)
                if 1 in mats:
                    for q in range(SUB):
                        xrecv(s, q).wait_recv()
                    own_product(1 - g, s)

    for q in range(SUB):
        zstep(1, 1, q)

    @pl.loop(2, n_a - 1)
    def _(d):
        for bb in range(2):
            for q in range(SUB):
                zstep(d, bb, q)
            take(d - 1, bb, (0, 1))

    ytok_in = remote(toks.at[ob, half_rows], toks.at[ob, half_rows], tok_s, tok_r, y_peer)
    ctok = remote(toks.at[ob, half_rows], toks.at[ob, half_rows], core_s, core_r, core_peer)
    yld.wait_recv()

    @pl.loop(1, n_sp)
    def _(k):
        tsend(k).wait_recv()

    pos_t = lax.broadcasted_iota(jnp.int32, (span, span), 0)
    pos_u = lax.broadcasted_iota(jnp.int32, (span, span), 1)
    later_mask = jnp.where(pos_u > pos_t, 1.0, 0.0).astype(F32)
    suffix = []
    for tb in range(2):
        inside = lax.dot_general(
            later_mask, lds[tb], (((1,), (1,)), ((), ())), precision=HIGH, preferred_element_type=F32
        )
        index = a * 2 + tb

        def add(k, total):
            return total + jnp.where(k > index, tots[k], 0.0)

        after = lax.fori_loop(0, n_sp, add, jnp.zeros(tots.shape[1:], F32))
        suffix.append(inside + after[0:1, :hs])
    row_hs = lax.broadcasted_iota(jnp.int32, (hs, cols), 0)
    lane_head = lax.broadcasted_iota(jnp.int32, (hs, cols), 1) // HEAD_DIM + b * (heads // 2)

    def prompt_weights(s):
        select = jnp.where(row_hs == lane_head * seqs + s, 1.0, 0.0).astype(F32)
        for tb in range(2):
            wts[tb, pl.ds(s * span, span), :] = jnp.exp(exact(suffix[tb], select))

    for q in range(SUB):
        zstep(n_a - 1, 0, q)
        for s in range(q, seqs, SUB):
            prompt_weights(s)
    take(n_a - 2, 0, (0, 1))
    for q in range(SUB):
        zstep(n_a - 1, 1, q)
        if q == SUB // 2 - 1:
            ytok_in.wait_recv()
            ctok.start()
    take(n_a - 2, 1, (0, 1))

    def partner_product(m):
        @pl.loop(0, rows // tile)
        def _(r):
            at = pl.ds(pl.multiple_of(r * tile, tile), tile)
            new = jnp.dot(toks[ob, at, :], w[m], preferred_element_type=F32)
            kv[m, ob, at, :] = new.astype(jnp.bfloat16)
            kv[m, b, at, :] = acc[m, at, :].astype(jnp.bfloat16)

    for bb in range(2):
        take(n_a - 1, bb, (0,))
    ctok.wait_recv()
    partner_product(g)
    for q in range(SUB):
        for m in range(2):
            @pl.when(g == m)
            def _():
                yw(1 - m, q).wait_recv()
    own_product(1 - g, a * 2 + ob)
    for bb in range(2):
        take(n_a - 1, bb, (1,))
    partner_product(1 - g)

    lane = lax.broadcasted_iota(jnp.int32, (span, 128), 1)
    first = lane % HEAD_DIM < HEAD_DIM // 2
    lane_out = lax.broadcasted_iota(jnp.int32, (HEAD_DIM, 128), 1)
    block = seqs * HEAD_DIM // n_a
    for s in range(seqs):
        for c0 in range(0, cols, 128):
            total = None
            for tb in range(2):
                at = pl.ds(s * span, span)
                u = kv[0, tb, at, pl.ds(c0, 128)].astype(F32)
                turned = jnp.where(first, pltpu.roll(u, 128 - 32, 1), pltpu.roll(u, 32, 1))
                spot = pl.ds(tb * span, span)
                rk = u * cos_ref[spot, :] + turned * sin_ref[spot, :]
                weighted = (rk * wts[tb, at, pl.ds(c0, 128)]).astype(jnp.bfloat16)
                term = lax.dot_general(
                    weighted, kv[1, tb, at, pl.ds(c0, 128)], (((0,), (0,)), ((), ())),
                    preferred_element_type=F32,
                )
                total = term if total is None else total + term
            both = jnp.where(lane_out < HEAD_DIM, total[:HEAD_DIM], total[HEAD_DIM:])
            part[pl.ds(s * HEAD_DIM, HEAD_DIM), pl.ds(c0, 128)] = both.astype(jnp.bfloat16)

    def block_of(k):
        return pl.ds(pl.multiple_of(k * block, block), block)

    def rs(k):
        to = lax.rem(a + k, n_a)
        return remote(part.at[block_of(to)], got.at[k], rs_s.at[k], rs_r.at[k], (g, to * 2 + b, tp))

    @pl.loop(1, n_a)
    def _(k):
        rs(k).start()

    @pl.loop(1, n_a)
    def _(k):
        rs(k).wait_recv()

    def gather(k, total):
        return total + got[k].astype(F32)

    reduced = lax.fori_loop(1, n_a, gather, part[block_of(a), :].astype(F32))
    full[b, block_of(a), :] = reduced.astype(jnp.bfloat16)

    def ag(k):
        here = full.at[b, block_of(a)]
        return remote(here, here, ag_s.at[k], ag_r.at[k], (g, lax.rem(a + k, n_a) * 2 + b, tp))

    def ag_in(k):
        here = full.at[b, block_of(lax.rem(a - k + n_a, n_a))]
        return remote(here, here, ag_s.at[k], ag_r.at[k], y_peer)

    def yg(k, bb):
        here = full.at[bb, block_of(lax.rem(a - k + n_a, n_a))]
        return remote(here, here, yg_s.at[k], yg_r.at[k], y_peer)

    @pl.loop(1, n_a)
    def _(k):
        ag(k).start()

    yg(0, b).start()

    @pl.loop(1, n_a)
    def _(k):
        ag_in(k).wait_recv()
        yg(k, b).start()

    @pl.loop(0, n_a)
    def _(k):
        yg(k, ob).wait_recv()

    for c0 in range(0, 2 * cols, 128):
        chunk = pl.ds(c0, 128)
        raws, states = [], []
        for s in range(seqs):
            at = pl.ds(s * HEAD_DIM, HEAD_DIM)
            summed = full[c0 // cols, at, pl.ds(c0 % cols, 128)].astype(F32)
            state = decay[s:s + 1, chunk] * summed + outer[at, chunk]
            raws.append(jnp.sum(qx[at, chunk] * state, axis=0, keepdims=True))
            states.append(state)
        out[chunk, :] = jnp.concatenate(states, axis=0).T
        raw = jnp.concatenate(raws, axis=0)
        center = exact(raw, same_head) * (1.0 / HEAD_DIM)
        off = raw - center
        spread = exact(off * off, same_head) * (1.0 / HEAD_DIM)
        read[:, chunk] = (off * lax.rsqrt(spread + 1e-06) * gain[:, chunk]).astype(jnp.bfloat16)

    @pl.loop(0, n_a)
    def _(k):
        yg(k, b).wait_send()

    @pl.loop(1, n_a)
    def _(k):
        ag(k).wait_send()
        rs(k).wait_send()

    @pl.loop(1, n_sp)
    def _(k):
        tsend(k).wait_send()

    ytok.wait_send()
    yld.wait_send()
    ctok.wait_send()
    for q in range(SUB):
        for m in range(2):
            yw(m, q).wait_send()
        for s in (sp, a * 2 + ob):
            @pl.when(a < n_a - 1)
            def _():
                zsend(s, q, True).wait_send()

            @pl.when(a > 0)
            def _():
                zsend(s, q, False).wait_send()

    @pl.loop(1, n_a)
    def _(d):
        for bb in range(2):
            for q in range(SUB):
                below = (a - d) * 2 + (b if bb == 0 else ob)
                above = (a + d) * 2 + (b if bb == 0 else ob)

                @pl.when(a - d >= 0)
                def _():
                    @pl.when(a < n_a - 1)
                    def _():
                        zsend(below, q, True).wait_send()

                    xsend(below, q).wait_send()

                @pl.when(a + d < n_a)
                def _():
                    @pl.when(a > 0)
                    def _():
                        zsend(above, q, False).wait_send()

                    xsend(above, q).wait_send()


def prompt_states(token_rows, key_weight, value_weight, decays, cos, sin, step, seqs, span, heads, n_sp):
    rows, width = token_rows.shape
    depth, whole = key_weight.shape
    cols = whole // 2
    n_a = n_sp // 2
    hs = heads * seqs
    state_rows = seqs * HEAD_DIM
    dma = pltpu.SemaphoreType.DMA
    bf16 = jnp.bfloat16
    hbm = pl.BlockSpec(memory_space=pl.ANY)
    vmem = pl.BlockSpec(memory_space=pltpu.VMEM)
    return pl.pallas_call(
        functools.partial(kernel, (n_sp, seqs, span, heads)),
        out_shape=(
            jax.ShapeDtypeStruct((whole, state_rows), F32),
            jax.ShapeDtypeStruct((seqs, whole), bf16),
        ),
        in_specs=[hbm] * 6 + [vmem] * 5,
        out_specs=(vmem, vmem),
        scratch_shapes=[
            pltpu.VMEM((2, rows, width), bf16),
            pltpu.VMEM((2, n_sp * depth, cols), bf16),
            pltpu.VMEM((2, 2, rows, cols), bf16),
            pltpu.VMEM((2, rows, cols), F32),
            pltpu.VMEM((2, hs, span), F32),
            pltpu.VMEM((n_sp, 8, 128), F32),
            pltpu.VMEM((state_rows, cols), bf16),
            pltpu.VMEM((n_a, state_rows // n_a, cols), bf16),
            pltpu.VMEM((2, state_rows, cols), bf16),
            pltpu.VMEM((2 * span, 128), F32),
            pltpu.VMEM((2 * span, 128), F32),
            pltpu.VMEM((2, 8, 128), F32),
            pltpu.VMEM((state_rows, whole), F32),
            pltpu.VMEM((state_rows, whole), F32),
            pltpu.VMEM((seqs, whole), F32),
            pltpu.VMEM((2, rows, cols), F32),
            dma((8,)), dma, dma, dma, dma,
            dma((2, SUB)), dma((2, SUB)),
            dma((n_sp, SUB)), dma((n_sp, SUB)), dma((n_sp, SUB)),
            dma((n_sp, SUB)), dma((n_sp, SUB)),
            dma, dma, dma((n_sp,)), dma((n_sp,)),
            dma((n_a,)), dma((n_a,)), dma((n_a,)), dma((n_a,)), dma((n_a,)), dma((n_a,)),
        ],
        compiler_params=pltpu.CompilerParams(
            collective_id=0, has_side_effects=True, vmem_limit_bytes=56 * 1024 * 1024
        ),
    )(token_rows, key_weight, value_weight, decays, cos, sin, *step)


def position_tables(length):
    half = HEAD_DIM // 2
    inverse = np.float32(10000.0) ** (-np.arange(half, dtype=np.float32) * np.float32(2.0 / HEAD_DIM))
    angles = np.arange(length + 8, dtype=np.float32)[:, None] * inverse[None, :].astype(np.float32)
    cosine = np.cos(angles.astype(np.float64)) * HEAD_DIM ** -0.5
    sine = np.sin(angles.astype(np.float64)) * HEAD_DIM ** -0.5
    cos = np.concatenate([cosine] * 4, axis=-1).astype(np.float32)
    sin = np.concatenate([-sine, sine] * 2, axis=-1).astype(np.float32)
    return cos, sin


def shards(
    tokens, key_weight, value_weight, log_decay, new_query, new_key, new_value, step_decay, norm_gain
):
    seqs, span, width = tokens.shape
    heads = key_weight.shape[1] // HEAD_DIM
    n_sp = lax.axis_size("sp")
    token_rows = tokens.reshape(seqs * span, width)
    decays = log_decay.reshape(heads * seqs, span)
    cos, sin = position_tables(span * n_sp)
    step = (new_query, new_key, new_value, step_decay.T, norm_gain.reshape(1, -1))
    state, read = prompt_states(
        token_rows, key_weight, value_weight, decays, jnp.asarray(cos), jnp.asarray(sin), step,
        seqs, span, heads, n_sp,
    )
    return (state.T.reshape(seqs * HEAD_DIM, heads, HEAD_DIM), read)


def solution(mesh):
    placed = (
        P("gr", "sp", None),
        P("sp", "tp"),
        P("sp", "tp"),
        P("tp", "gr", "sp"),
        P("gr", "tp"),
        P("gr", "tp"),
        P("gr", "tp"),
        P("tp", "gr"),
        P("tp"),
    )
    return jax.shard_map(
        shards,
        mesh=mesh,
        in_specs=placed,
        out_specs=(P("gr", "tp", None), P("gr", "tp")),
        check_vma=False,
    )
```
